32 devices in a mesh: grp: 2 (over y), sp: 4 (over z), dp: 4 (over x, core).
Axes of the slice: x: 2, y: 2, z: 4, core: 2. Of those that a mesh axis runs over, the one named last changes fastest.
Arguments:
- tokens: bfloat16 [8, 640, 2048], P(('grp', 'dp'), 'sp'), parts along dimension 0, may hold values from -6 to 6
- query_weight: bfloat16 [2048, 1024], P('dp'), may hold values from -0.125 to 0.125
- key_weight: bfloat16 [2048, 256], P('dp'), may hold values from -0.125 to 0.125
- value_weight: bfloat16 [2048, 256], P('dp'), may hold values from -0.125 to 0.125
- out_weight: bfloat16 [1024, 2048], P(None, 'dp'), may hold values from -0.1875 to 0.1875
- query_gain: float32 [64], replicated, may hold values from 0.28 to 6
- key_gain: float32 [64], replicated, may hold values from 0.28 to 6
Outputs:
- mixed: bfloat16 [8, 640, 2048], P(('grp', 'dp'), 'sp'), parts along dimension 0
The draws below stay inside these ranges and needn't reach their ends.
There are 2 independent parts, one for each index of `grp`. The reference program is written for one: setup_inputs(seed, part) draws one part's arguments, and reference() takes and returns one part's arrays. A program takes and returns all parts, laid end to end along the dimension named above; an argument that names none is the same for every part. Nothing has to cross between parts.
All inputs are finite; a program needn't handle non-finite values.
Results may differ from the reference program's by a relative error of at most 0.006.
The reference program's roundings to bfloat16 on the way count: a program that leaves them out, or rounds other values in their place, can miss the bound.
Values may be sent and summed in bfloat16 or wider, within the bound.
A program may use at most 64 MiB of HBM per device.

```python
import jax
import jax.numpy as jnp
from jax import lax

D = 2048
HEADS = 16
KV_HEADS = 4
HEAD_DIM = 64
GRID_W = 64
SEQ_LEN = 640
SEQS = 4


def gain_values(key):
    return 1.0 + 0.18 * jnp.clip(jax.random.normal(key, (HEAD_DIM,), jnp.float32), -4.0, 4.0)


def draw_query_gain(key, part):
    return gain_values(jax.random.fold_in(key, 11))


def draw_key_gain(key, part):
    return gain_values(jax.random.fold_in(key, 23))


def level_of(rng, dims, split, least, largest):
    factor_of, own = 1.0, jax.random.fold_in(rng, 6)
    for position, blocks in split:
        steps = jnp.exp(jax.random.uniform(jax.random.fold_in(own, position), (blocks,), jnp.float32, least / len(split), largest / len(split)))
        factor_of = factor_of * jnp.repeat(steps, dims[position] // blocks).reshape([-1 if axis == position else 1 for axis in range(len(dims))])
    return factor_of


def gaussian(rng, shape, spread, bound, pieces=(), kind=jnp.bfloat16):
    values = jax.random.normal(rng, shape, jnp.float32) * spread
    if len(pieces) > 0:
        values = level_of(rng, shape, pieces, -0.22, 0.18) * values
    return jnp.clip(values, min=-bound, max=bound).astype(kind)


def setup_inputs(seed: int = 0, part: int = 0) -> dict:
    splits = jax.random.split(jax.random.key(seed), 8)
    part_splits = jax.random.split(jax.random.fold_in(splits[7], part), 8)
    tokens = gaussian(part_splits[0], (SEQS, SEQ_LEN, D), 1.0, 6.0, ((0, 4), (1, 4)))
    query_weight = gaussian(splits[1], (D, HEADS * HEAD_DIM), D ** -0.5, 0.125, ((0, 4),))
    key_weight = gaussian(splits[2], (D, KV_HEADS * HEAD_DIM), D ** -0.5, 0.125, ((0, 4),))
    value_weight = gaussian(splits[3], (D, KV_HEADS * HEAD_DIM), D ** -0.5, 0.125, ((0, 4),))
    out_weight = gaussian(splits[4], (HEADS * HEAD_DIM, D), (HEADS * HEAD_DIM) ** -0.5, 0.1875, ((1, 4),))
    query_gain = draw_query_gain(jax.random.fold_in(splits[7], 71), part)
    key_gain = draw_key_gain(jax.random.fold_in(splits[7], 71), part)
    return dict(tokens=tokens, query_weight=query_weight, key_weight=key_weight, value_weight=value_weight, out_weight=out_weight, query_gain=query_gain, key_gain=key_gain)


theta_base = 10000.0
norm_eps = 1e-06

def rotary_tables(positions):
    quarter = HEAD_DIM // 4
    inverse = theta_base ** (-jnp.arange(quarter, dtype=jnp.float32) / quarter)
    grid_rows = (positions // GRID_W).astype(jnp.float32)
    grid_cols = (positions % GRID_W).astype(jnp.float32)
    angles = jnp.concatenate([grid_rows[:, None] * inverse, grid_cols[:, None] * inverse], axis=-1)
    return (jnp.cos(angles), jnp.sin(angles))

def norm_rotate(raw, gain, cosine, sine):
    scaled = raw * lax.rsqrt(lax.optimization_barrier(jnp.mean(raw * raw, axis=-1, keepdims=True)) + norm_eps) * gain
    half = HEAD_DIM // 2
    first_half = scaled[..., :half]
    second_half = scaled[..., half:]
    cosine = cosine[:, None, :]
    sine = sine[:, None, :]
    turned = jnp.concatenate([first_half * cosine - second_half * sine, second_half * cosine + first_half * sine], axis=-1)
    return turned.astype(jnp.bfloat16)

def reference(tokens, query_weight, key_weight, value_weight, out_weight, query_gain, key_gain):
    length = tokens.shape[1]
    per_kv = HEADS // KV_HEADS
    cosine, sine = rotary_tables(jnp.arange(length, dtype=jnp.int32))
    scale = HEAD_DIM ** (-0.5)

    def one_sequence(rows_in):
        raw_q = jnp.dot(rows_in, query_weight, preferred_element_type=jnp.float32).reshape(length, HEADS, HEAD_DIM)
        raw_k = jnp.dot(rows_in, key_weight, preferred_element_type=jnp.float32).reshape(length, KV_HEADS, HEAD_DIM)
        values = jnp.dot(rows_in, value_weight, preferred_element_type=jnp.float32).astype(jnp.bfloat16)
        queries = norm_rotate(raw_q, query_gain, cosine, sine)
        keys = norm_rotate(raw_k, key_gain, cosine, sine)
        query_heads = queries.reshape(length, KV_HEADS, per_kv, HEAD_DIM).transpose(1, 0, 2, 3)
        key_heads = keys.transpose(1, 0, 2)
        value_heads = values.reshape(length, KV_HEADS, HEAD_DIM).transpose(1, 0, 2)

        def one_head(operands):
            head_q, head_k, head_v = operands
            scores = jnp.einsum('qgd,sd->gqs', head_q.astype(jnp.float32), head_k.astype(jnp.float32)) * scale
            top = lax.optimization_barrier(jnp.max(scores, axis=-1, keepdims=True))
            weights = jnp.exp(scores - top)
            probs = (weights / lax.optimization_barrier(jnp.sum(weights, axis=-1, keepdims=True))).astype(jnp.bfloat16)
            return jnp.einsum('gqs,sd->qgd', probs.astype(jnp.float32), head_v.astype(jnp.float32)).astype(jnp.bfloat16)
        attended = lax.map(one_head, (query_heads, key_heads, value_heads))
        attended = attended.transpose(1, 0, 2, 3).reshape(length, HEADS * HEAD_DIM)
        return jnp.dot(attended, out_weight, preferred_element_type=jnp.float32).astype(jnp.bfloat16)
    return lax.map(one_sequence, tokens)
```

```python
import functools

import jax
import jax.numpy as jnp
from jax import lax
from jax.experimental import pallas as pl
from jax.experimental.pallas import tpu as pltpu
from jax.sharding import PartitionSpec as P

HEADS = 16
KV_HEADS = 4
HEAD_DIM = 64
GRID_W = 64
LANES = 128

theta_base = 10000.0
norm_eps = 1e-06

BF = jnp.bfloat16
F32 = jnp.float32
MESH = pl.DeviceIdType.MESH


def rotary_tables(positions):
    quarter = HEAD_DIM // 4
    inverse = theta_base ** (-jnp.arange(quarter, dtype=F32) / quarter)
    grid_rows = (positions // GRID_W).astype(F32)
    grid_cols = (positions % GRID_W).astype(F32)
    angles = jnp.concatenate([grid_rows[:, None] * inverse, grid_cols[:, None] * inverse], axis=-1)
    return (jnp.cos(angles), jnp.sin(angles))


def dot(a, b):
    return jnp.dot(a, b, preferred_element_type=F32)


def kernel(n, groups, seqs, cuts, tok, wk, wv, wq, wo, cos, sin, gq, gk, out,
           fk, fv, fq, fo, kv, acc_k, acc_v, acc_q, qs, k2, v2, att,
           xs, xr, ys, yr, os_, or_, cxs, cxr, cys, cyr, zs, zr):
    d = lax.axis_index("dp")
    g = lax.axis_index("grp")
    s = lax.axis_index("sp")
    chips = n // 2
    mate = d + 1 - 2 * lax.rem(d, 2)
    own = (wk, wv, wq, wo)
    full = (fk, fv, fq, fo)
    rows = tok.shape[0]

    def hop(j):
        return lax.rem(d + 2 * j, n)

    def back(dev, j):
        return lax.rem(dev + n - 2 * j, n)

    def color(i):
        return lax.rem(g + groups - i, groups)

    barrier = pltpu.get_barrier_semaphore()
    for j in range(1, chips):
        pl.semaphore_signal(barrier, inc=1, device_id={"dp": hop(j)}, device_id_type=MESH)
    for i in range(1, groups):
        pl.semaphore_signal(barrier, inc=1, device_id={"grp": lax.rem(g + i, groups)}, device_id_type=MESH)
    for i in range(1, seqs):
        pl.semaphore_signal(barrier, inc=1, device_id={"sp": lax.rem(s + i, seqs)}, device_id_type=MESH)
    pl.semaphore_signal(barrier, inc=1, device_id={"dp": mate}, device_id_type=MESH)
    pl.semaphore_wait(barrier, chips - 1 + groups - 1 + seqs - 1 + 1)

    sent = []

    def send(src, dst, ssem, rsem, where):
        copy = pltpu.make_async_remote_copy(
            src_ref=src, dst_ref=dst, send_sem=ssem, recv_sem=rsem, device_id=where, device_id_type=MESH)
        copy.start()
        sent.append(copy)

    def arrive(dst, ssem, rsem):
        pltpu.make_async_remote_copy(
            src_ref=dst, dst_ref=dst, send_sem=ssem, recv_sem=rsem,
            device_id={"dp": mate}, device_id_type=MESH).wait_recv()

    pieces = [(kind, cut) for kind in range(4) for cut in range(cuts[kind])]

    def span(p, which):
        kind, cut = pieces[p]
        size = own[kind].shape[0] // groups // cuts[kind]
        start = which * (own[kind].shape[0] // groups) + cut * size
        return pl.ds(pl.multiple_of(start, 16), size)

    for p in range(len(pieces)):
        kind = pieces[p][0]
        for j in range(1, chips):
            part = span(p, g)
            send(own[kind].at[part], full[kind].at[d, part], xs.at[j - 1, p], xr.at[j - 1, p], {"dp": hop(j)})
    for kind in range(4):
        send(own[kind], full[kind].at[d], os_.at[kind], or_.at[kind], {"dp": mate})

    def step_x(p):
        kind = pieces[p][0]
        part = span(p, g)
        for j in range(1, chips):
            owner = back(d, j)
            here = full[kind].at[owner, part]
            arrive(here, xs.at[j - 1, p], xr.at[j - 1, p])
            for i in range(1, groups):
                send(here, here, ys.at[j - 1, i - 1, p], yr.at[j - 1, i - 1, p],
                     {"grp": lax.rem(g + i, groups)})
            send(here, here, cxs.at[j - 1, p], cxr.at[j - 1, p], {"dp": mate})

    def step_y(p):
        kind = pieces[p][0]
        for j in range(1, chips):
            owner = back(d, j)
            for i in range(1, groups):
                here = full[kind].at[owner, span(p, color(i))]
                arrive(here, ys.at[j - 1, i - 1, p], yr.at[j - 1, i - 1, p])
                send(here, here, cys.at[j - 1, i - 1, p], cyr.at[j - 1, i - 1, p], {"dp": mate})

    def step_own(kind):
        arrive(full[kind].at[mate], os_.at[kind], or_.at[kind])

    def step_c(p):
        kind = pieces[p][0]
        for j in range(1, chips):
            owner = back(mate, j)
            arrive(full[kind].at[owner, span(p, g)], cxs.at[j - 1, p], cxr.at[j - 1, p])
            for i in range(1, groups):
                arrive(full[kind].at[owner, span(p, color(i))],
                       cys.at[j - 1, i - 1, p], cyr.at[j - 1, i - 1, p])

    depth = wq.shape[0]

    def columns(owner):
        return pl.ds(pl.multiple_of(owner * depth, LANES), depth)

    def first(acc, ref):
        acc[...] = dot(tok[:, columns(d)], ref[...])

    def more(acc, ref, owner):
        acc[...] += dot(tok[:, columns(owner)], ref[owner])

    first(acc_k, wk)
    first(acc_v, wv)
    first(acc_q, wq)

    lane = lax.broadcasted_iota(jnp.int32, (rows, LANES), 1)
    low_half = lax.rem(lane, HEAD_DIM) < HEAD_DIM // 2
    low_head = lane < HEAD_DIM
    square_r = lax.broadcasted_iota(jnp.int32, (LANES, LANES), 0)
    square_c = lax.broadcasted_iota(jnp.int32, (LANES, LANES), 1)
    same_head = jnp.where(square_r // HEAD_DIM == square_c // HEAD_DIM, 1.0, 0.0).astype(BF)

    def norm_rotate(raw, gain):
        sq = raw * raw
        high = sq.astype(BF)
        low = (sq - high.astype(F32)).astype(BF)
        total = dot(high, same_head) + dot(low, same_head)
        scaled = raw * lax.rsqrt(total * (1.0 / HEAD_DIM) + norm_eps) * gain
        other = jnp.where(low_half, pltpu.roll(scaled, LANES - HEAD_DIM // 2, 1),
                          pltpu.roll(scaled, HEAD_DIM // 2, 1))
        return scaled * cos[...] + other * sin[...]

    others = [(d, j) for j in range(1, chips)] + [(mate, j) for j in range(1, chips)]

    def finish_kv():
        for acc, kind in ((acc_k, 0), (acc_v, 1)):
            for p in range(len(pieces)):
                if pieces[p][0] == kind:
                    step_c(p)
            for dev, j in others:
                more(acc, full[kind], back(dev, j))
        width = wk.shape[1]
        for t in range(width // LANES):
            cols = pl.ds(t * LANES, LANES)
            kv[s, :, cols] = norm_rotate(acc_k[:, cols], gk[...]).astype(BF)
        kv[s, :, pl.ds(width, width)] = acc_v[...].astype(BF)
        for i in range(1, seqs):
            send(kv.at[s], kv.at[s], zs.at[i - 1], zr.at[i - 1], {"sp": lax.rem(s + i, seqs)})

    def finish_q():
        for p in range(len(pieces)):
            if pieces[p][0] == 2:
                step_c(p)
        for dev, j in others:
            more(acc_q, fq, back(dev, j))
        for t in range(wq.shape[1] // LANES):
            turned = norm_rotate(acc_q[:, pl.ds(t * LANES, LANES)], gq[...]).astype(BF).astype(F32)
            turned = turned * HEAD_DIM ** (-0.5)
            qs[t, pl.ds(0, rows), :] = jnp.where(low_head, turned, 0.0).astype(BF)
            qs[t, pl.ds(rows, rows), :] = jnp.where(low_head, 0.0, turned).astype(BF)

    def gather_kv():
        for i in range(1, seqs):
            arrive(kv.at[lax.rem(s + seqs - i, seqs)], zs.at[i - 1], zr.at[i - 1])
        width = wk.shape[1]
        for h in range(KV_HEADS):
            offset = (h % 2) * HEAD_DIM
            twice = jnp.where(square_r == offset + lax.rem(square_c, HEAD_DIM), 1.0, 0.0).astype(BF)
            base = (h // 2) * LANES
            for src, dst in ((base, k2), (width + base, v2)):
                block = kv[:, :, pl.ds(src, LANES)].reshape(seqs * rows, LANES)
                dst[h] = dot(block, twice).astype(BF)

    tiles = wq.shape[1] // LANES

    def attend(lo, hi):
        def body(t, carry):
            h = t // (tiles // KV_HEADS)
            scores = lax.dot_general(qs[t], k2[h], (((1,), (1,)), ((), ())), preferred_element_type=F32)
            top = jnp.max(scores, axis=-1, keepdims=True)
            weights = jnp.exp(scores - top)
            inverse = 1.0 / jnp.sum(weights, axis=-1, keepdims=True)
            mixed = dot((weights * inverse).astype(BF), v2[h])
            att[:, pl.ds(pl.multiple_of(t * LANES, LANES), LANES)] = jnp.where(
                low_head, mixed[:rows], mixed[rows:]).astype(BF)
            return carry
        lax.fori_loop(lo, hi, body, 0)

    def project(ref, owner):
        width = wo.shape[1]
        out[:, pl.ds(pl.multiple_of(owner * width, LANES), width)] = dot(att[...], ref).astype(BF)

    total = len(pieces)
    kv_end = cuts[0] + cuts[1]
    q_end = kv_end + cuts[2]
    left = cuts[3]
    done = 0
    for p in range(total):
        step_x(p)
        if p >= 1:
            step_y(p - 1)
        if p == 1:
            step_own(0)
            more(acc_k, fk, mate)
            step_own(1)
            more(acc_v, fv, mate)
        if p == kv_end:
            finish_kv()
            step_own(2)
            more(acc_q, fq, mate)
        if p == q_end:
            finish_q()
        if p > q_end:
            if p == q_end + 1:
                gather_kv()
            upto = tiles * (p - q_end) // left
            attend(done, upto)
            done = upto
    step_y(total - 1)
    attend(done, tiles)
    project(wo[...], d)
    step_own(3)
    project(fo[mate], mate)
    for j in range(1, chips):
        project(fo[back(d, j)], back(d, j))
    for p in range(q_end, total):
        step_c(p)
    for j in range(1, chips):
        project(fo[back(mate, j)], back(mate, j))
    for copy in sent:
        copy.wait_send()


def shards(n, groups, seqs, tokens, query_weight, key_weight, value_weight, out_weight, query_gain, key_gain):
    rows, width = tokens.shape[1], tokens.shape[2]
    local = tokens.reshape(rows, width)
    positions = lax.axis_index("sp") * rows + jnp.arange(rows, dtype=jnp.int32)
    cosine, sine = rotary_tables(positions)
    cos = jnp.concatenate([cosine] * 4, axis=1)
    sin = jnp.concatenate([-sine, sine] * 2, axis=1)
    gq = jnp.tile(query_gain, 2).reshape(1, LANES)
    gk = jnp.tile(key_gain, 2).reshape(1, LANES)
    cuts = (1, 1, 4, 4)
    count = sum(cuts)
    chips = n // 2
    kvw, qw = key_weight.shape[1], query_weight.shape[1]
    length = rows * seqs
    dma = pltpu.SemaphoreType.DMA
    vmem = pl.BlockSpec(memory_space=pltpu.VMEM)
    result = pl.pallas_call(
        functools.partial(kernel, n, groups, seqs, cuts),
        out_shape=jax.ShapeDtypeStruct((rows, width), BF),
        in_specs=[vmem] * 9,
        out_specs=vmem,
        scratch_shapes=[
            pltpu.VMEM((n,) + key_weight.shape, BF),
            pltpu.VMEM((n,) + value_weight.shape, BF),
            pltpu.VMEM((n,) + query_weight.shape, BF),
            pltpu.VMEM((n,) + out_weight.shape, BF),
            pltpu.VMEM((seqs, rows, 2 * kvw), BF),
            pltpu.VMEM((rows, kvw), F32),
            pltpu.VMEM((rows, kvw), F32),
            pltpu.VMEM((rows, qw), F32),
            pltpu.VMEM((qw // LANES, 2 * rows, LANES), BF),
            pltpu.VMEM((KV_HEADS, length, LANES), BF),
            pltpu.VMEM((KV_HEADS, length, LANES), BF),
            pltpu.VMEM((rows, qw), BF),
            dma((chips - 1, count)), dma((chips - 1, count)),
            dma((chips - 1, groups - 1, count)), dma((chips - 1, groups - 1, count)),
            dma((4,)), dma((4,)),
            dma((chips - 1, count)), dma((chips - 1, count)),
            dma((chips - 1, groups - 1, count)), dma((chips - 1, groups - 1, count)),
            dma((seqs - 1,)), dma((seqs - 1,)),
        ],
        compiler_params=pltpu.CompilerParams(
            collective_id=0, has_side_effects=True, vmem_limit_bytes=60 * 2 ** 20),
    )(local, key_weight, value_weight, query_weight, out_weight, cos, sin, gq, gk)
    return result.reshape(1, rows, width)


def solution(mesh):
    in_specs = (
        P(("grp", "dp"), "sp", None),
        P("dp", None),
        P("dp", None),
        P("dp", None),
        P(None, "dp"),
        P(),
        P(),
    )
    out_specs = P(("grp", "dp"), "sp", None)
    body = functools.partial(shards, mesh.shape["dp"], mesh.shape["grp"], mesh.shape["sp"])
    return jax.shard_map(body, mesh=mesh, in_specs=in_specs, out_specs=out_specs, check_vma=False)
```

```python
import functools
import math

import jax
import jax.numpy as jnp
from jax import lax
from jax.experimental import pallas as pl
from jax.experimental.pallas import tpu as pltpu
from jax.sharding import PartitionSpec as P

HEADS = 16
KV_HEADS = 4
HEAD_DIM = 64
GRID_W = 64
LANES = 128

theta_base = 10000.0
norm_eps = 1e-06

BF = jnp.bfloat16
F32 = jnp.float32
MESH = pl.DeviceIdType.MESH


def rotary_tables(start, rows):
    quarter = HEAD_DIM // 4
    lane = lax.broadcasted_iota(jnp.int32, (rows, LANES), 1)
    position = start + lax.broadcasted_iota(jnp.int32, (rows, LANES), 0)
    step = lax.rem(lane, quarter).astype(F32)
    inverse = jnp.exp(step * (-math.log(theta_base) / quarter))
    grid_row = lax.div(position, GRID_W)
    grid_col = lax.rem(position, GRID_W)
    place = jnp.where(lax.rem(lane, 2 * quarter) < quarter, grid_row, grid_col).astype(F32)
    angles = place * inverse
    sine = jnp.sin(angles)
    return jnp.cos(angles), jnp.where(lax.rem(lane, HEAD_DIM) < HEAD_DIM // 2, -sine, sine)


def dot(a, b):
    return jnp.dot(a, b, preferred_element_type=F32)


def kernel(n, groups, seqs, cuts, order, tok, wk, wv, wq, wo, gq, gk, out,
           fk, fv, fq, fo, cos, sin, kv, acc_k, acc_v, acc_q, qs, k2, v2, att,
           xs, xr, ys, yr, ps, pr, os_, or_, cxs, cxr, zs, zr):
    d = lax.axis_index("dp")
    g = lax.axis_index("grp")
    s = lax.axis_index("sp")
    chips = n // 2
    mate = d + 1 - 2 * lax.rem(d, 2)
    own = (wk, wv, wq, wo)
    full = (fk, fv, fq, fo)
    rows = tok.shape[0]

    def hop(j):
        return lax.rem(d + 2 * j, n)

    def back(dev, j):
        return lax.rem(dev + n - 2 * j, n)

    def other(i):
        return i + 1 - 2 * lax.rem(i, 2)

    e = lax.rem(s, 2)
    colors = (2 * g + e, 2 * other(g) + e, 2 * g + other(e), 2 * other(g) + other(e))

    barrier = pltpu.get_barrier_semaphore()
    for j in range(1, chips):
        pl.semaphore_signal(barrier, inc=1, device_id={"dp": hop(j)}, device_id_type=MESH)
    for i in range(1, groups):
        pl.semaphore_signal(barrier, inc=1, device_id={"grp": lax.rem(g + i, groups)}, device_id_type=MESH)
    for i in range(1, seqs):
        pl.semaphore_signal(barrier, inc=1, device_id={"sp": lax.rem(s + i, seqs)}, device_id_type=MESH)
    pl.semaphore_signal(barrier, inc=1, device_id={"dp": mate}, device_id_type=MESH)
    pl.semaphore_wait(barrier, chips - 1 + groups - 1 + seqs - 1 + 1)

    sent = []

    def send(src, dst, ssem, rsem, where):
        copy = pltpu.make_async_remote_copy(
            src_ref=src, dst_ref=dst, send_sem=ssem, recv_sem=rsem, device_id=where, device_id_type=MESH)
        copy.start()
        sent.append(copy)

    def arrive(dst, ssem, rsem):
        pltpu.make_async_remote_copy(
            src_ref=dst, dst_ref=dst, send_sem=ssem, recv_sem=rsem,
            device_id={"dp": mate}, device_id_type=MESH).wait_recv()

    pieces = [(kind, cut) for kind in range(4) for cut in range(cuts[kind])]

    def block(ref, p, color):
        kind, cut = pieces[p]
        quarter = own[kind].shape[0] // 4
        size = quarter // cuts[kind]
        start = color * quarter + cut * size
        return ref.at[pl.ds(pl.multiple_of(start, 16), size)]

    def held(owner, p, rel):
        return block(full[pieces[p][0]].at[owner], p, colors[rel])

    ahead = 4

    def x_copy(index, j):
        p, rel = order[index]
        return pltpu.make_async_remote_copy(
            src_ref=block(own[pieces[p][0]], p, colors[rel]), dst_ref=held(d, p, rel),
            send_sem=xs.at[j - 1, rel, p], recv_sem=xr.at[j - 1, rel, p],
            device_id={"dp": hop(j)}, device_id_type=MESH)

    for index in range(min(ahead, len(order))):
        for j in range(1, chips):
            x_copy(index, j).start()
    for kind in range(4):
        send(own[kind], full[kind].at[d], os_.at[kind], or_.at[kind], {"dp": mate})

    def to_mate(here, j, rel, p):
        send(here, here, cxs.at[j - 1, rel, p], cxr.at[j - 1, rel, p], {"dp": mate})

    def step_x(p, rel):
        index = order.index((p, rel))
        for j in range(1, chips):
            here = held(back(d, j), p, rel)
            arrive(here, xs.at[j - 1, rel, p], xr.at[j - 1, rel, p])
            if rel != 3:
                send(here, here, ys.at[j - 1, rel // 2, p], yr.at[j - 1, rel // 2, p], {"grp": other(g)})
            if rel == 0 and (p, 2) not in order:
                send(here, here, ps.at[j - 1, p], pr.at[j - 1, p], {"sp": other(s)})
            to_mate(here, j, rel, p)
        for j in range(1, chips):
            x_copy(index, j).wait_send()
            if index + ahead < len(order):
                x_copy(index + ahead, j).start()

    def step_y(p, rel=1):
        for j in range(1, chips):
            here = held(back(d, j), p, rel)
            arrive(here, ys.at[j - 1, rel // 3, p], yr.at[j - 1, rel // 3, p])
            to_mate(here, j, rel, p)

    def step_z(p):
        for j in range(1, chips):
            here = held(back(d, j), p, 2)
            arrive(here, ps.at[j - 1, p], pr.at[j - 1, p])
            if (p, 3) not in order:
                send(here, here, ys.at[j - 1, 1, p], yr.at[j - 1, 1, p], {"grp": other(g)})
            to_mate(here, j, 2, p)

    def step_own(kind):
        arrive(full[kind].at[mate], os_.at[kind], or_.at[kind])

    def step_c(p):
        for j in range(1, chips):
            for rel in range(4):
                arrive(held(back(mate, j), p, rel), cxs.at[j - 1, rel, p], cxr.at[j - 1, rel, p])

    depth = wq.shape[0]

    def columns(owner):
        return pl.ds(pl.multiple_of(owner * depth, LANES), depth)

    def first(acc, ref):
        acc[...] = dot(tok[:, columns(d)], ref[...])

    def more(acc, ref, owner):
        acc[...] += dot(tok[:, columns(owner)], ref[owner])

    cos[...], sin[...] = rotary_tables(s * rows, rows)
    first(acc_k, wk)
    first(acc_v, wv)
    first(acc_q, wq)

    lane = lax.broadcasted_iota(jnp.int32, (rows, LANES), 1)
    low_half = lax.rem(lane, HEAD_DIM) < HEAD_DIM // 2
    low_head = lane < HEAD_DIM
    square_r = lax.broadcasted_iota(jnp.int32, (LANES, LANES), 0)
    square_c = lax.broadcasted_iota(jnp.int32, (LANES, LANES), 1)
    same_head = jnp.where(square_r // HEAD_DIM == square_c // HEAD_DIM, 1.0, 0.0).astype(BF)

    gain_k = jnp.concatenate([gk[...]] * 2, axis=1)
    gain_q = jnp.concatenate([gq[...]] * 2, axis=1)

    def norm_rotate(raw, gain):
        sq = raw * raw
        high = sq.astype(BF)
        low = (sq - high.astype(F32)).astype(BF)
        total = dot(high, same_head) + dot(low, same_head)
        scaled = raw * lax.rsqrt(total * (1.0 / HEAD_DIM) + norm_eps) * gain
        other = jnp.where(low_half, pltpu.roll(scaled, LANES - HEAD_DIM // 2, 1),
                          pltpu.roll(scaled, HEAD_DIM // 2, 1))
        return scaled * cos[...] + other * sin[...]

    others = [(d, j) for j in range(1, chips)] + [(mate, j) for j in range(1, chips)]

    held_back = []

    def relay(k):
        for way in range(2):
            sign = 2 * way - 1
            source, target = s + sign * k, s - sign
            here = (source >= 0) & (source < seqs)
            there = here & (target >= 0) & (target < seqs)
            slot = jnp.clip(source, 0, seqs - 1)
            goal = jnp.clip(target, 0, seqs - 1)
            width = kv.shape[2] // 2
            for half in range(2):
                ref = kv.at[slot, :, pl.ds(half * width, width)]
                if k > 0:
                    @pl.when(here)
                    def _():
                        arrive(ref, zs.at[way, half, k - 1], zr.at[way, half, k - 1])
                if k < seqs - 1:
                    copy = pltpu.make_async_remote_copy(
                        src_ref=ref, dst_ref=ref, send_sem=zs.at[way, half, k], recv_sem=zr.at[way, half, k],
                        device_id={"sp": goal}, device_id_type=MESH)
                    pl.when(there)(copy.start)
                    held_back.append((there, copy))

    def finish_kv():
        for acc, kind in ((acc_k, 0), (acc_v, 1)):
            for p in range(len(pieces)):
                if pieces[p][0] == kind:
                    step_c(p)
            for dev, j in others:
                more(acc, full[kind], back(dev, j))
        width = wk.shape[1]
        for t in range(width // LANES):
            cols = pl.ds(t * LANES, LANES)
            kv[s, :, cols] = norm_rotate(acc_k[:, cols], gain_k).astype(BF)
        kv[s, :, pl.ds(width, width)] = acc_v[...].astype(BF)
        relay(0)

    def finish_q():
        for p in range(len(pieces)):
            if pieces[p][0] == 2:
                step_c(p)
        for dev, j in others:
            more(acc_q, fq, back(dev, j))
        for t in range(wq.shape[1] // LANES):
            turned = norm_rotate(acc_q[:, pl.ds(t * LANES, LANES)], gain_q).astype(BF).astype(F32)
            turned = turned * HEAD_DIM ** (-0.5)
            qs[t, pl.ds(0, rows), :] = jnp.where(low_head, turned, 0.0).astype(BF)
            qs[t, pl.ds(rows, rows), :] = jnp.where(low_head, 0.0, turned).astype(BF)

    def gather_kv():
        width = wk.shape[1]
        for h in range(KV_HEADS):
            offset = (h % 2) * HEAD_DIM
            twice = jnp.where(square_r == offset + lax.rem(square_c, HEAD_DIM), 1.0, 0.0).astype(BF)
            base = (h // 2) * LANES
            for src, dst in ((base, k2), (width + base, v2)):
                both = kv[:, :, pl.ds(src, LANES)].reshape(seqs * rows, LANES)
                dst[h] = dot(both, twice).astype(BF)

    tiles = wq.shape[1] // LANES

    def attend(lo, hi):
        def body(t, carry):
            h = t // (tiles // KV_HEADS)
            scores = lax.dot_general(qs[t], k2[h], (((1,), (1,)), ((), ())), preferred_element_type=F32)
            top = jnp.max(scores, axis=-1, keepdims=True)
            weights = jnp.exp(scores - top)
            inverse = 1.0 / jnp.sum(weights, axis=-1, keepdims=True)
            mixed = dot((weights * inverse).astype(BF), v2[h])
            att[:, pl.ds(pl.multiple_of(t * LANES, LANES), LANES)] = jnp.where(
                low_head, mixed[:rows], mixed[rows:]).astype(BF)
            return carry
        lax.fori_loop(lo, hi, body, 0)

    def project(ref, owner):
        width = wo.shape[1]
        out[:, pl.ds(pl.multiple_of(owner * width, LANES), width)] = dot(att[...], ref).astype(BF)

    middle = max(1, (seqs - 1) // 3)
    step_x(0, 0)
    step_x(1, 0)
    step_x(0, 3)
    step_y(0, 1)
    step_z(0)
    step_x(1, 3)
    step_own(0)
    more(acc_k, fk, mate)
    step_own(1)
    more(acc_v, fv, mate)
    step_y(1, 1)
    step_z(1)
    step_x(2, 0)
    finish_kv()
    step_x(3, 0)
    step_own(2)
    more(acc_q, fq, mate)
    step_y(2, 1)
    step_z(2)
    for k in range(1, 1 + middle):
        relay(k)
    step_x(3, 3)
    step_y(3, 1)
    step_x(4, 0)
    step_z(3)
    step_y(2, 3)
    for k in range(1 + middle, 1 + 2 * middle):
        relay(k)
    step_x(5, 0)
    step_y(4, 1)
    finish_q()
    step_x(5, 2)
    step_z(4)
    for k in range(1 + 2 * middle, seqs):
        relay(k)
    step_x(4, 3)
    gather_kv()
    attend(tiles * 0 // 8, tiles * 2 // 8)
    step_y(5, 1)
    attend(tiles * 2 // 8, tiles * 4 // 8)
    step_y(5, 3)
    attend(tiles * 4 // 8, tiles * 8 // 8)
    project(wo[...], d)
    step_own(3)
    project(fo[mate], mate)
    for j in range(1, chips):
        project(fo[back(d, j)], back(d, j))
    for p in range(4, len(pieces)):
        step_c(p)
    for j in range(1, chips):
        project(fo[back(mate, j)], back(mate, j))
    for copy in sent:
        copy.wait_send()
    for there, copy in held_back:
        pl.when(there)(copy.wait_send)


def shards(n, groups, seqs, tokens, query_weight, key_weight, value_weight, out_weight, query_gain, key_gain):
    rows, width = tokens.shape[1], tokens.shape[2]
    local = tokens.reshape(rows, width)
    cuts = (1, 1, 2, 2)
    order = ((0, 0), (1, 0), (0, 3), (1, 3), (2, 0), (3, 0), (3, 3), (4, 0), (5, 0), (5, 2), (4, 3))
    count = sum(cuts)
    chips = n // 2
    kvw, qw = key_weight.shape[1], query_weight.shape[1]
    length = rows * seqs
    dma = pltpu.SemaphoreType.DMA
    vmem = pl.BlockSpec(memory_space=pltpu.VMEM)
    result = pl.pallas_call(
        functools.partial(kernel, n, groups, seqs, cuts, order),
        out_shape=jax.ShapeDtypeStruct((rows, width), BF),
        in_specs=[vmem] * 7,
        out_specs=vmem,
        scratch_shapes=[
            pltpu.VMEM((n,) + key_weight.shape, BF),
            pltpu.VMEM((n,) + value_weight.shape, BF),
            pltpu.VMEM((n,) + query_weight.shape, BF),
            pltpu.VMEM((n,) + out_weight.shape, BF),
            pltpu.VMEM((rows, LANES), F32),
            pltpu.VMEM((rows, LANES), F32),
            pltpu.VMEM((seqs, rows, 2 * kvw), BF),
            pltpu.VMEM((rows, kvw), F32),
            pltpu.VMEM((rows, kvw), F32),
            pltpu.VMEM((rows, qw), F32),
            pltpu.VMEM((qw // LANES, 2 * rows, LANES), BF),
            pltpu.VMEM((KV_HEADS, length, LANES), BF),
            pltpu.VMEM((KV_HEADS, length, LANES), BF),
            pltpu.VMEM((rows, qw), BF),
            dma((chips - 1, 4, count)), dma((chips - 1, 4, count)),
            dma((chips - 1, 2, count)), dma((chips - 1, 2, count)),
            dma((chips - 1, count)), dma((chips - 1, count)),
            dma((4,)), dma((4,)),
            dma((chips - 1, 4, count)), dma((chips - 1, 4, count)),
            dma((2, 2, seqs - 1)), dma((2, 2, seqs - 1)),
        ],
        compiler_params=pltpu.CompilerParams(
            collective_id=0, has_side_effects=True, vmem_limit_bytes=60 * 2 ** 20),
    )(local, key_weight, value_weight, query_weight, out_weight,
      query_gain.reshape(1, HEAD_DIM), key_gain.reshape(1, HEAD_DIM))
    return result.reshape(1, rows, width)


def solution(mesh):
    in_specs = (
        P(("grp", "dp"), "sp", None),
        P("dp", None),
        P("dp", None),
        P("dp", None),
        P(None, "dp"),
        P(),
        P(),
    )
    out_specs = P(("grp", "dp"), "sp", None)
    body = functools.partial(shards, mesh.shape["dp"], mesh.shape["grp"], mesh.shape["sp"])
    return jax.shard_map(body, mesh=mesh, in_specs=in_specs, out_specs=out_specs, check_vma=False)
```

```python
import functools
import math

import jax
import jax.numpy as jnp
from jax import lax
from jax.experimental import pallas as pl
from jax.experimental.pallas import tpu as pltpu
from jax.sharding import PartitionSpec as P

HEADS = 16
KV_HEADS = 4
HEAD_DIM = 64
GRID_W = 64
LANES = 128

theta_base = 10000.0
norm_eps = 1e-06

BF = jnp.bfloat16
F32 = jnp.float32
MESH = pl.DeviceIdType.MESH


def rotary_tables(start, rows):
    quarter = HEAD_DIM // 4
    lane = lax.broadcasted_iota(jnp.int32, (rows, LANES), 1)
    position = start + lax.broadcasted_iota(jnp.int32, (rows, LANES), 0)
    step = lax.rem(lane, quarter).astype(F32)
    inverse = jnp.exp(step * (-math.log(theta_base) / quarter))
    grid_row = lax.div(position, GRID_W)
    grid_col = lax.rem(position, GRID_W)
    place = jnp.where(lax.rem(lane, 2 * quarter) < quarter, grid_row, grid_col).astype(F32)
    angles = place * inverse
    sine = jnp.sin(angles)
    return jnp.cos(angles), jnp.where(lax.rem(lane, HEAD_DIM) < HEAD_DIM // 2, -sine, sine)


def dot(a, b):
    return jnp.dot(a, b, preferred_element_type=F32)


def kernel(n, groups, seqs, cuts, order, tok, wk, wv, wq, wo, gq, gk, out,
           fk, fv, fq, fo, cos, sin, kv, acc_k, acc_v, acc_q, qs, k2, v2, att,
           xs, xr, ys, yr, ps, pr, os_, or_, cxs, cxr, zs, zr):
    d = lax.axis_index("dp")
    g = lax.axis_index("grp")
    s = lax.axis_index("sp")
    chips = n // 2
    mate = d + 1 - 2 * lax.rem(d, 2)
    own = (wk, wv, wq, wo)
    full = (fk, fv, fq, fo)
    rows = tok.shape[0]

    def hop(j):
        return lax.rem(d + 2 * j, n)

    def back(dev, j):
        return lax.rem(dev + n - 2 * j, n)

    def other(i):
        return i + 1 - 2 * lax.rem(i, 2)

    e = lax.rem(s, 2)
    colors = (2 * g + e, 2 * other(g) + e, 2 * g + other(e), 2 * other(g) + other(e))

    barrier = pltpu.get_barrier_semaphore()
    for j in range(1, chips):
        pl.semaphore_signal(barrier, inc=1, device_id={"dp": hop(j)}, device_id_type=MESH)
    for i in range(1, groups):
        pl.semaphore_signal(barrier, inc=1, device_id={"grp": lax.rem(g + i, groups)}, device_id_type=MESH)
    for i in range(1, seqs):
        pl.semaphore_signal(barrier, inc=1, device_id={"sp": lax.rem(s + i, seqs)}, device_id_type=MESH)
    pl.semaphore_signal(barrier, inc=1, device_id={"dp": mate}, device_id_type=MESH)
    pl.semaphore_wait(barrier, chips - 1 + groups - 1 + seqs - 1 + 1)

    sent = []

    def send(src, dst, ssem, rsem, where):
        copy = pltpu.make_async_remote_copy(
            src_ref=src, dst_ref=dst, send_sem=ssem, recv_sem=rsem, device_id=where, device_id_type=MESH)
        copy.start()
        sent.append(copy)

    def arrive(dst, ssem, rsem):
        pltpu.make_async_remote_copy(
            src_ref=dst, dst_ref=dst, send_sem=ssem, recv_sem=rsem,
            device_id={"dp": mate}, device_id_type=MESH).wait_recv()

    pieces = [(kind, cut) for kind in range(4) for cut in range(cuts[kind])]

    def block(ref, p, color):
        kind, cut = pieces[p]
        quarter = own[kind].shape[0] // 4
        size = quarter // cuts[kind]
        start = color * quarter + cut * size
        return ref.at[pl.ds(pl.multiple_of(start, 16), size)]

    def held(owner, p, rel):
        return block(full[pieces[p][0]].at[owner], p, colors[rel])

    ahead = 4

    def x_copy(index, j):
        p, rel = order[index]
        return pltpu.make_async_remote_copy(
            src_ref=block(own[pieces[p][0]], p, colors[rel]), dst_ref=held(d, p, rel),
            send_sem=xs.at[j - 1, rel, p], recv_sem=xr.at[j - 1, rel, p],
            device_id={"dp": hop(j)}, device_id_type=MESH)

    for index in range(min(ahead, len(order))):
        for j in range(1, chips):
            x_copy(index, j).start()
    for kind in range(4):
        send(own[kind], full[kind].at[d], os_.at[kind], or_.at[kind], {"dp": mate})

    def to_mate(here, j, rel, p):
        send(here, here, cxs.at[j - 1, rel, p], cxr.at[j - 1, rel, p], {"dp": mate})

    def step_x(p, rel):
        index = order.index((p, rel))
        for j in range(1, chips):
            here = held(back(d, j), p, rel)
            arrive(here, xs.at[j - 1, rel, p], xr.at[j - 1, rel, p])
            if rel != 3:
                send(here, here, ys.at[j - 1, rel // 2, p], yr.at[j - 1, rel // 2, p], {"grp": other(g)})
            if rel == 0 and (p, 2) not in order:
                send(here, here, ps.at[j - 1, p], pr.at[j - 1, p], {"sp": other(s)})
            to_mate(here, j, rel, p)
        for j in range(1, chips):
            x_copy(index, j).wait_send()
            if index + ahead < len(order):
                x_copy(index + ahead, j).start()

    def step_y(p, rel=1):
        for j in range(1, chips):
            here = held(back(d, j), p, rel)
            arrive(here, ys.at[j - 1, rel // 3, p], yr.at[j - 1, rel // 3, p])
            to_mate(here, j, rel, p)

    def step_z(p):
        for j in range(1, chips):
            here = held(back(d, j), p, 2)
            arrive(here, ps.at[j - 1, p], pr.at[j - 1, p])
            if (p, 3) not in order:
                send(here, here, ys.at[j - 1, 1, p], yr.at[j - 1, 1, p], {"grp": other(g)})
            to_mate(here, j, 2, p)

    def step_own(kind):
        arrive(full[kind].at[mate], os_.at[kind], or_.at[kind])

    def step_c(p):
        for j in range(1, chips):
            for rel in range(4):
                arrive(held(back(mate, j), p, rel), cxs.at[j - 1, rel, p], cxr.at[j - 1, rel, p])

    depth = wq.shape[0]

    def columns(owner):
        return pl.ds(pl.multiple_of(owner * depth, LANES), depth)

    def first(acc, ref):
        acc[...] = dot(tok[:, columns(d)], ref[...])

    def more(acc, ref, owner):
        acc[...] += dot(tok[:, columns(owner)], ref[owner])

    cos[...], sin[...] = rotary_tables(s * rows, rows)
    first(acc_k, wk)
    first(acc_v, wv)
    first(acc_q, wq)

    lane = lax.broadcasted_iota(jnp.int32, (rows, LANES), 1)
    low_half = lax.rem(lane, HEAD_DIM) < HEAD_DIM // 2
    low_head = lane < HEAD_DIM
    square_r = lax.broadcasted_iota(jnp.int32, (LANES, LANES), 0)
    square_c = lax.broadcasted_iota(jnp.int32, (LANES, LANES), 1)
    same_head = jnp.where(square_r // HEAD_DIM == square_c // HEAD_DIM, 1.0, 0.0).astype(BF)

    gain_k = jnp.concatenate([gk[...]] * 2, axis=1)
    gain_q = jnp.concatenate([gq[...]] * 2, axis=1)

    def norm_rotate(raw, gain):
        sq = raw * raw
        high = sq.astype(BF)
        low = (sq - high.astype(F32)).astype(BF)
        total = dot(high, same_head) + dot(low, same_head)
        scaled = raw * lax.rsqrt(total * (1.0 / HEAD_DIM) + norm_eps) * gain
        other = jnp.where(low_half, pltpu.roll(scaled, LANES - HEAD_DIM // 2, 1),
                          pltpu.roll(scaled, HEAD_DIM // 2, 1))
        return scaled * cos[...] + other * sin[...]

    others = [(d, j) for j in range(1, chips)] + [(mate, j) for j in range(1, chips)]

    held_back = []

    def relay(k):
        for way in range(2):
            sign = 2 * way - 1
            source, target = s + sign * k, s - sign
            here = (source >= 0) & (source < seqs)
            there = here & (target >= 0) & (target < seqs)
            slot = jnp.clip(source, 0, seqs - 1)
            goal = jnp.clip(target, 0, seqs - 1)
            width = kv.shape[2] // 2
            for half in range(2):
                ref = kv.at[slot, :, pl.ds(half * width, width)]
                if k > 0:
                    @pl.when(here)
                    def _():
                        arrive(ref, zs.at[way, half, k - 1], zr.at[way, half, k - 1])
                if k < seqs - 1:
                    copy = pltpu.make_async_remote_copy(
                        src_ref=ref, dst_ref=ref, send_sem=zs.at[way, half, k], recv_sem=zr.at[way, half, k],
                        device_id={"sp": goal}, device_id_type=MESH)
                    pl.when(there)(copy.start)
                    held_back.append((there, copy))

    def finish_kv():
        for acc, kind in ((acc_k, 0), (acc_v, 1)):
            for p in range(len(pieces)):
                if pieces[p][0] == kind:
                    step_c(p)
            for dev, j in others:
                more(acc, full[kind], back(dev, j))
        width = wk.shape[1]
        for t in range(width // LANES):
            cols = pl.ds(t * LANES, LANES)
            kv[s, :, cols] = norm_rotate(acc_k[:, cols], gain_k).astype(BF)
        kv[s, :, pl.ds(width, width)] = acc_v[...].astype(BF)
        relay(0)

    def finish_q():
        for p in range(len(pieces)):
            if pieces[p][0] == 2:
                step_c(p)
        for dev, j in others:
            more(acc_q, fq, back(dev, j))
        for t in range(wq.shape[1] // LANES):
            turned = norm_rotate(acc_q[:, pl.ds(t * LANES, LANES)], gain_q).astype(BF).astype(F32)
            turned = turned * HEAD_DIM ** (-0.5)
            qs[t, pl.ds(0, rows), :] = jnp.where(low_head, turned, 0.0).astype(BF)
            qs[t, pl.ds(rows, rows), :] = jnp.where(low_head, 0.0, turned).astype(BF)

    def gather_kv():
        width = wk.shape[1]
        for h in range(KV_HEADS):
            offset = (h % 2) * HEAD_DIM
            twice = jnp.where(square_r == offset + lax.rem(square_c, HEAD_DIM), 1.0, 0.0).astype(BF)
            base = (h // 2) * LANES
            for src, dst in ((base, k2), (width + base, v2)):
                both = kv[:, :, pl.ds(src, LANES)].reshape(seqs * rows, LANES)
                dst[h] = dot(both, twice).astype(BF)

    tiles = wq.shape[1] // LANES

    def attend(lo, hi):
        def body(t, carry):
            h = t // (tiles // KV_HEADS)
            scores = lax.dot_general(qs[t], k2[h], (((1,), (1,)), ((), ())), preferred_element_type=F32)
            top = jnp.max(scores, axis=-1, keepdims=True)
            weights = jnp.exp(scores - top)
            inverse = 1.0 / jnp.sum(weights, axis=-1, keepdims=True)
            mixed = dot((weights * inverse).astype(BF), v2[h])
            att[:, pl.ds(pl.multiple_of(t * LANES, LANES), LANES)] = jnp.where(
                low_head, mixed[:rows], mixed[rows:]).astype(BF)
            return carry
        lax.fori_loop(lo, hi, body, 0, unroll=True)

    def project(ref, owner):
        width = wo.shape[1]
        out[:, pl.ds(pl.multiple_of(owner * width, LANES), width)] = dot(att[...], ref).astype(BF)

    middle = max(1, (seqs - 1) // 3)
    step_x(0, 0)
    step_x(1, 0)
    step_x(0, 3)
    step_y(0, 1)
    step_z(0)
    step_x(1, 3)
    step_own(0)
    more(acc_k, fk, mate)
    step_own(1)
    more(acc_v, fv, mate)
    step_y(1, 1)
    step_z(1)
    step_x(2, 0)
    finish_kv()
    step_x(3, 0)
    step_own(2)
    more(acc_q, fq, mate)
    step_y(2, 1)
    step_z(2)
    for k in range(1, 1 + middle):
        relay(k)
    step_x(3, 3)
    step_y(3, 1)
    step_x(4, 0)
    step_z(3)
    step_y(2, 3)
    for k in range(1 + middle, 1 + 2 * middle):
        relay(k)
    step_x(5, 0)
    step_y(4, 1)
    finish_q()
    step_x(5, 2)
    step_z(4)
    for k in range(1 + 2 * middle, seqs):
        relay(k)
    step_x(4, 3)
    gather_kv()
    attend(tiles * 0 // 8, tiles * 2 // 8)
    step_y(5, 1)
    attend(tiles * 2 // 8, tiles * 4 // 8)
    step_y(5, 3)
    attend(tiles * 4 // 8, tiles * 8 // 8)
    project(wo[...], d)
    step_own(3)
    project(fo[mate], mate)
    for j in range(1, chips):
        project(fo[back(d, j)], back(d, j))
    for p in range(4, len(pieces)):
        step_c(p)
    for j in range(1, chips):
        project(fo[back(mate, j)], back(mate, j))
    for copy in sent:
        copy.wait_send()
    for there, copy in held_back:
        pl.when(there)(copy.wait_send)


def shards(n, groups, seqs, tokens, query_weight, key_weight, value_weight, out_weight, query_gain, key_gain):
    rows, width = tokens.shape[1], tokens.shape[2]
    local = tokens.reshape(rows, width)
    cuts = (1, 1, 2, 2)
    order = ((0, 0), (1, 0), (0, 3), (1, 3), (2, 0), (3, 0), (3, 3), (4, 0), (5, 0), (5, 2), (4, 3))
    count = sum(cuts)
    chips = n // 2
    kvw, qw = key_weight.shape[1], query_weight.shape[1]
    length = rows * seqs
    dma = pltpu.SemaphoreType.DMA
    vmem = pl.BlockSpec(memory_space=pltpu.VMEM)
    result = pl.pallas_call(
        functools.partial(kernel, n, groups, seqs, cuts, order),
        out_shape=jax.ShapeDtypeStruct((rows, width), BF),
        in_specs=[vmem] * 7,
        out_specs=vmem,
        scratch_shapes=[
            pltpu.VMEM((n,) + key_weight.shape, BF),
            pltpu.VMEM((n,) + value_weight.shape, BF),
            pltpu.VMEM((n,) + query_weight.shape, BF),
            pltpu.VMEM((n,) + out_weight.shape, BF),
            pltpu.VMEM((rows, LANES), F32),
            pltpu.VMEM((rows, LANES), F32),
            pltpu.VMEM((seqs, rows, 2 * kvw), BF),
            pltpu.VMEM((rows, kvw), F32),
            pltpu.VMEM((rows, kvw), F32),
            pltpu.VMEM((rows, qw), F32),
            pltpu.VMEM((qw // LANES, 2 * rows, LANES), BF),
            pltpu.VMEM((KV_HEADS, length, LANES), BF),
            pltpu.VMEM((KV_HEADS, length, LANES), BF),
            pltpu.VMEM((rows, qw), BF),
            dma((chips - 1, 4, count)), dma((chips - 1, 4, count)),
            dma((chips - 1, 2, count)), dma((chips - 1, 2, count)),
            dma((chips - 1, count)), dma((chips - 1, count)),
            dma((4,)), dma((4,)),
            dma((chips - 1, 4, count)), dma((chips - 1, 4, count)),
            dma((2, 2, seqs - 1)), dma((2, 2, seqs - 1)),
        ],
        compiler_params=pltpu.CompilerParams(
            collective_id=0, has_side_effects=True, vmem_limit_bytes=60 * 2 ** 20),
    )(local, key_weight, value_weight, query_weight, out_weight,
      query_gain.reshape(1, HEAD_DIM), key_gain.reshape(1, HEAD_DIM))
    return result.reshape(1, rows, width)


def solution(mesh):
    in_specs = (
        P(("grp", "dp"), "sp", None),
        P("dp", None),
        P("dp", None),
        P("dp", None),
        P(None, "dp"),
        P(),
        P(),
    )
    out_specs = P(("grp", "dp"), "sp", None)
    body = functools.partial(shards, mesh.shape["dp"], mesh.shape["grp"], mesh.shape["sp"])
    return jax.shard_map(body, mesh=mesh, in_specs=in_specs, out_specs=out_specs, check_vma=False)
```
